32 devices in a mesh: sp: 16 (over z, y, core), tp: 2 (over x).
Axes of the slice: x: 2, y: 2, z: 4, core: 2. Of those that a mesh axis runs over, the one named last changes fastest.
Arguments:
- tokens: bfloat16 [6144, 2048], P('sp', 'tp'), may hold values from -60 to 60
- pre_gain: bfloat16 [2048], P('tp'), may hold values from 0.099609375 to 1.8984375
- w_query: bfloat16 [2048, 1024], P('sp', 'tp'), may hold values from -1 to 1
- w_key: bfloat16 [2048, 1024], P('sp', 'tp'), may hold values from -1 to 1
- w_value: bfloat16 [2048, 1024], P('sp', 'tp'), may hold values from -0.125 to 0.125
- w_pool: bfloat16 [2048, 1024], P('sp', 'tp'), may hold values from -0.125 to 0.125
- lambdas: float32 [8], P('tp'), may hold values from 0.3 to 0.8
- sub_gain: float32 [128], replicated, may hold values from 0.1 to 1.9
- group_weight: bfloat16 [8, 128, 128], P('tp'), may hold values from -0.5 to 0.5
- pool_scale: float32 [1024], P('tp'), may hold values from 0.1 to 1.9
- w_out: bfloat16 [2048, 2048], P('tp', 'sp'), may hold values from -0.125 to 0.125
Outputs:
- mixed_out: bfloat16 [6144, 2048], P(('sp', 'tp'))
The draws below stay inside these ranges and needn't reach their ends.
All inputs are finite; a program needn't handle non-finite values.
Results may differ from the reference program's by a relative error of at most 0.015.
Values may be sent and summed in bfloat16 or wider, within the bound.
A program may use at most 128 MiB of HBM per device.

```python
import math
import jax
import jax.numpy as jnp
import numpy as np
from jax import lax

D = 2048
HEADS = 8
HDIM = 64
VDIM = 128
GROUPS = 8
GDIM = 128
TOKENS = 6144


def draw_tokens(key, part):
    noise = jax.random.normal(jax.random.fold_in(key, 11), (TOKENS, D), jnp.float32)
    row_scale = jnp.exp(jax.random.uniform(jax.random.fold_in(key, 12), (TOKENS, 1), jnp.float32, 0.0, math.log(10.0)))
    column_rise = 1.1 * jnp.arange(D, dtype=jnp.float32)[None, :] / D
    column_scale = jnp.exp(jax.random.uniform(jax.random.fold_in(key, 13), (1, D), jnp.float32, -0.7, 0.7) + column_rise)
    result = noise * row_scale * column_scale
    return jnp.clip(result, -60.0, 60.0).astype(jnp.bfloat16)


def query_key_pair(key):
    columns = HEADS * 2 * HDIM
    spread = math.sqrt(2.0 / D)
    first = jax.random.normal(jax.random.fold_in(key, 21), (D, columns), jnp.float32) * spread
    second = jax.random.normal(jax.random.fold_in(key, 22), (D, columns), jnp.float32) * spread
    return (jnp.clip(first, -1.0, 1.0), jnp.clip(second, -1.0, 1.0))


def draw_w_query(key, part):
    return query_key_pair(key)[0].astype(jnp.bfloat16)


def draw_w_key(key, part):
    return query_key_pair(key)[1].astype(jnp.bfloat16)


def level_of(rng, shape, split, least, high):
    factor_of, own = 1.0, jax.random.fold_in(rng, 6)
    for dim, shards_of in split:
        heights = jnp.exp(jax.random.uniform(jax.random.fold_in(own, dim), (shards_of,), jnp.float32, least / len(split), high / len(split)))
        factor_of = factor_of * jnp.repeat(heights, shape[dim] // shards_of).reshape([-1 if axis == dim else 1 for axis in range(len(shape))])
    return factor_of


def bell_draw(stream_key, extent, width, reach, shards=(), held_as=jnp.bfloat16):
    values = jax.random.normal(stream_key, extent, jnp.float32) * width
    if len(shards) > 0:
        values = level_of(stream_key, extent, shards, -0.22, 0.18) * values
    return jnp.clip(values, min=-reach, max=reach).astype(held_as)


def setup_inputs(seed: int = 0) -> dict:
    splits = jax.random.split(jax.random.key(seed), 12)
    tokens = draw_tokens(jax.random.fold_in(splits[11], 71), 0)
    pre_gain = jnp.clip(1.0 + 0.18 * jax.random.normal(splits[1], (D,), jnp.float32), 0.099609375, 1.8984375).astype(jnp.bfloat16)
    w_query = draw_w_query(jax.random.fold_in(splits[11], 71), 0)
    w_key = draw_w_key(jax.random.fold_in(splits[11], 71), 0)
    w_value = bell_draw(splits[4], (D, HEADS * VDIM), D ** -0.5, 0.125, ((0, 16), (1, 2)))
    w_pool = bell_draw(splits[5], (D, GROUPS * GDIM), D ** -0.5, 0.125, ((0, 16), (1, 2)))
    lambdas = jnp.clip(0.3 + 0.5 * jax.random.uniform(splits[6], (HEADS,), jnp.float32) ** level_of(splits[6], (HEADS,), ((0, 2),), -0.2, 0.2), 0.3, 0.8)
    sub_gain = jnp.clip(1.0 + 0.18 * jax.random.normal(splits[7], (VDIM,), jnp.float32), 0.1, 1.9)
    group_weight = bell_draw(splits[8], (GROUPS, GDIM, GDIM), GDIM ** -0.5, 0.5, ((0, 2),))
    pool_scale = jnp.clip(1.0 + 0.18 * jax.random.normal(splits[9], (GROUPS * GDIM,), jnp.float32), 0.1, 1.9)
    w_out = bell_draw(splits[10], (HEADS * (VDIM + GDIM), D), (HEADS * (VDIM + GDIM)) ** -0.5, 0.125, ((0, 2), (1, 16)))
    return {"tokens": tokens, "pre_gain": pre_gain, "w_query": w_query, "w_key": w_key, "w_value": w_value, "w_pool": w_pool, "lambdas": lambdas, "sub_gain": sub_gain, "group_weight": group_weight, "pool_scale": pool_scale, "w_out": w_out}


EPSILON = 1e-06
WINDOWS = (2, 4, 8, 16)
RIM_ROWS = 15

def head_block(query_head, key_head, value_head, weight_two, first_row):
    block_len = query_head.shape[0]
    key_len = key_head.shape[0]
    score_scale = 1.0 / math.sqrt(HDIM)
    scores = jnp.einsum('qmd,kmd->mqk', query_head.astype(jnp.float32), key_head.astype(jnp.float32)) * score_scale
    allowed = jnp.arange(key_len, dtype=jnp.int32)[None, :] <= (first_row + jnp.arange(block_len, dtype=jnp.int32))[:, None]
    scores = jnp.where(allowed[None], scores, -jnp.inf)
    row_max = lax.optimization_barrier(jnp.max(scores, axis=-1, keepdims=True))
    expo = jnp.where(allowed[None], jnp.exp(scores - row_max), 0.0)
    row_sum = lax.optimization_barrier(jnp.sum(expo, axis=-1))
    rounded = lax.optimization_barrier(expo.astype(jnp.bfloat16)).astype(jnp.float32)
    weighted = jnp.einsum('mqk,kd->mqd', rounded, value_head.astype(jnp.float32))
    head_mix = weighted[0] / row_sum[0][:, None] - weight_two * weighted[1] / row_sum[1][:, None]
    return head_mix

def reference(tokens, pre_gain, w_query, w_key, w_value, w_pool, lambdas, sub_gain, group_weight, pool_scale, w_out):
    features = tokens.astype(jnp.float32)
    inverse = lax.rsqrt(lax.optimization_barrier(jnp.mean(features * features, axis=1, keepdims=True)) + EPSILON)
    scaled = (features * pre_gain.astype(jnp.float32)).astype(jnp.bfloat16)

    def project(weight):
        return (jnp.dot(scaled, weight, preferred_element_type=jnp.float32) * inverse).astype(jnp.bfloat16)
    queries = project(w_query).reshape(TOKENS, HEADS, 2, HDIM)
    key_rows = project(w_key).reshape(TOKENS, HEADS, 2, HDIM)
    values = project(w_value).reshape(TOKENS, HEADS, VDIM)
    pool_in = project(w_pool)
    block_len = math.gcd(TOKENS, 512)
    pieces = []
    for block_index in range(TOKENS // block_len):
        first_row = block_index * block_len
        key_len = first_row + block_len
        query_heads = jnp.transpose(queries[first_row:key_len], (1, 0, 2, 3))
        key_heads = jnp.transpose(key_rows[:key_len], (1, 0, 2, 3))
        value_heads = jnp.transpose(values[:key_len], (1, 0, 2))

        def one_head(packed):
            return head_block(packed[0], packed[1], packed[2], packed[3], first_row)
        mixed_heads = lax.map(one_head, (query_heads, key_heads, value_heads, lambdas))
        mean_sq = lax.optimization_barrier(jnp.mean(mixed_heads * mixed_heads, axis=-1, keepdims=True))
        normed = mixed_heads * lax.rsqrt(mean_sq + EPSILON) * sub_gain
        pieces.append(jnp.transpose(normed, (1, 0, 2)).astype(jnp.bfloat16))
    attention = jnp.concatenate(pieces, axis=0)
    pool_float = pool_in.astype(jnp.float32)
    extended = jnp.concatenate([jnp.zeros((RIM_ROWS, GROUPS * GDIM), jnp.float32), pool_float], axis=0)
    running = jnp.concatenate([jnp.zeros((1, GROUPS * GDIM), jnp.float32), jnp.cumsum(extended, axis=0)], axis=0)
    running_top = running[RIM_ROWS + 1:]
    positions = jnp.arange(TOKENS, dtype=jnp.int32)
    window_of_column = np.repeat(np.arange(GROUPS) % len(WINDOWS), GDIM)
    average = jnp.zeros_like(running_top)
    for window_slot, window_span in enumerate(WINDOWS):
        running_low = running[RIM_ROWS + 1 - window_span:RIM_ROWS + 1 - window_span + TOKENS]
        window_count = jnp.minimum(positions + 1, window_span).astype(jnp.float32)
        average = average + jnp.where(window_of_column[None, :] == window_slot, (running_top - running_low) / window_count[:, None], 0.0)
    differ = (average - pool_float).astype(jnp.bfloat16).reshape(TOKENS, GROUPS, GDIM)
    pooled = jnp.einsum('tgc,gcd->tgd', differ.astype(jnp.float32), group_weight.astype(jnp.float32))
    pooled = (pooled * pool_scale.reshape(GROUPS, GDIM)).astype(jnp.bfloat16)
    branch = jnp.concatenate([attention, pooled], axis=2).reshape(TOKENS, HEADS * (VDIM + GDIM))
    return jnp.dot(branch, w_out, preferred_element_type=jnp.float32).astype(jnp.bfloat16)
```

```python
import functools
import math

import jax
import jax.numpy as jnp
from jax import lax
from jax.experimental import pallas as pl
from jax.experimental.pallas import tpu as pltpu
from jax.sharding import PartitionSpec as P

EPSILON = 1e-06
NEG_LARGE = -1e30
WINDOWS = (2, 4, 8, 16)
RIM_ROWS = 15


def passed_along(block, axis, distance):
    devices = range(lax.axis_size(axis))
    route = [(i - distance, i) for i in devices if i - distance in devices]
    return lax.ppermute(block, axis, route)


def attend(inner, vdim, hdim, member_ref, lam_ref, q_ref, kv_ref, gain_ref, out_ref, acc_ref, max_ref):
    rows = q_ref.shape[1]
    block = pl.program_id(0)
    last = block * inner + member_ref[0]
    scale = 1.0 / math.sqrt(hdim)
    queries = (q_ref[0].astype(jnp.float32) * scale).astype(jnp.bfloat16)
    maps = (queries[:, :hdim], queries[:, hdim:])
    ones = jnp.ones((rows, vdim), jnp.bfloat16)
    acc_ref[...] = jnp.zeros_like(acc_ref)
    max_ref[...] = jnp.full_like(max_ref, NEG_LARGE)

    def step(g, masked):
        keys_values = kv_ref[lax.rem(g, inner), lax.div(g, inner)]
        values = jnp.concatenate([keys_values[:, 2 * hdim :], ones], axis=1)
        for m in range(2):
            keys = keys_values[:, m * hdim : (m + 1) * hdim]
            scores = lax.dot_general(
                maps[m], keys, (((1,), (1,)), ((), ())), preferred_element_type=jnp.float32
            )
            if masked:
                row = lax.broadcasted_iota(jnp.int32, scores.shape, 0)
                col = lax.broadcasted_iota(jnp.int32, scores.shape, 1)
                scores = jnp.where(col <= row, scores, NEG_LARGE)
            old_max = max_ref[m]
            new_max = jnp.maximum(old_max, jnp.max(scores, axis=1, keepdims=True))
            factor = jnp.exp(old_max - new_max)
            expo = jnp.exp(scores - new_max[:, :1])
            acc_ref[m] = acc_ref[m] * factor[:, :1] + jnp.dot(
                expo.astype(jnp.bfloat16), values, preferred_element_type=jnp.float32
            )
            max_ref[m] = new_max

    def body(g, carry):
        step(g, False)
        return carry

    lax.fori_loop(0, last, body, 0)
    step(last, True)
    first = acc_ref[0]
    second = acc_ref[1]
    mix = first[:, :vdim] / first[:, vdim:] - lam_ref[0] * (second[:, :vdim] / second[:, vdim:])
    mean_sq = jnp.mean(mix * mix, axis=1, keepdims=True)
    out_ref[0] = (mix * lax.rsqrt(mean_sq + EPSILON) * gain_ref[...]).astype(jnp.bfloat16)


def flash(q, kv, member, lam, sub_gain):
    inner, outer, rows, width = kv.shape
    qdim = q.shape[-1]
    vdim = width - qdim
    smem = pl.BlockSpec(memory_space=pltpu.SMEM)
    work = outer * rows * outer * rows * inner
    return pl.pallas_call(
        functools.partial(attend, inner, vdim, qdim // 2),
        grid=(outer,),
        out_shape=jax.ShapeDtypeStruct((outer, rows, vdim), jnp.bfloat16),
        in_specs=[
            smem,
            smem,
            pl.BlockSpec((1, rows, qdim), lambda b: (b, 0, 0)),
            pl.BlockSpec(memory_space=pltpu.VMEM),
            pl.BlockSpec(memory_space=pltpu.VMEM),
        ],
        out_specs=pl.BlockSpec((1, rows, vdim), lambda b: (b, 0, 0)),
        scratch_shapes=[
            pltpu.VMEM((2, rows, 2 * vdim), jnp.float32),
            pltpu.VMEM((2, rows, 128), jnp.float32),
        ],
        compiler_params=pltpu.CompilerParams(vmem_limit_bytes=56 * 2**20),
        cost_estimate=pl.CostEstimate(
            flops=4 * work * vdim, bytes_accessed=kv.size * 2, transcendentals=work
        ),
    )(member, lam, q, kv, sub_gain.reshape(1, -1))


def trailing(x, window_ids, group_dim):
    column_window = jnp.repeat(window_ids, group_dim)[None, :]
    running = x
    picked = jnp.zeros_like(x)
    for slot, span in enumerate(WINDOWS):
        half = span // 2
        running = running + jnp.pad(running[:-half], ((half, 0), (0, 0)))
        picked = jnp.where(column_window == slot, running, picked)
    return picked


def local(
    tokens,
    pre_gain,
    w_query,
    w_key,
    w_value,
    w_pool,
    lambdas,
    sub_gain,
    group_weight,
    pool_scale,
    w_out,
):
    n_tp = lax.axis_size("tp")
    n_sp = lax.axis_size("sp")
    tp = lax.axis_index("tp")
    sp = lax.axis_index("sp")
    tok_rows = tokens.shape[0]
    model_width = tokens.shape[1] * n_tp
    heads = lambdas.shape[0]
    qdim = w_query.shape[1] // heads
    vdim = w_value.shape[1] // heads
    groups = group_weight.shape[0]
    group_dim = group_weight.shape[1]
    head_width = 2 * qdim + vdim
    outer = math.gcd(n_sp, heads)
    inner = n_sp // outer
    per_device = heads // outer

    pieces = []
    for h in range(heads):
        pieces += [
            w_query[:, h * qdim : (h + 1) * qdim],
            w_key[:, h * qdim : (h + 1) * qdim],
            w_value[:, h * vdim : (h + 1) * vdim],
        ]
    w_cat = jnp.concatenate(pieces + [w_pool], axis=1)
    w_in = lax.all_gather(w_cat, "sp", axis=0, tiled=True)
    w_out_rows = lax.all_gather(w_out, "sp", axis=1, tiled=True)

    features = tokens.astype(jnp.float32)
    mine = (features * pre_gain.astype(jnp.float32)[None, :]).astype(jnp.bfloat16)
    squares = jnp.sum(features * features, axis=1, keepdims=True)
    if n_tp == 2:
        swap = [(0, 1), (1, 0)]
        theirs = lax.ppermute(mine, "tp", swap)
        squares = squares + lax.ppermute(squares, "tp", swap)
        scaled = jnp.concatenate(
            [jnp.where(tp == 0, mine, theirs), jnp.where(tp == 0, theirs, mine)], axis=1
        )
    else:
        scaled = lax.all_gather(mine, "tp", axis=1, tiled=True)
        squares = lax.psum(squares, "tp")
    inverse = lax.rsqrt(squares / model_width + EPSILON)
    projected = (jnp.dot(scaled, w_in, preferred_element_type=jnp.float32) * inverse).astype(
        jnp.bfloat16
    )

    by_head = jnp.stack(
        [projected[:, h * head_width : (h + 1) * head_width] for h in range(heads)], axis=0
    )
    across = [[o * inner + i for o in range(outer)] for i in range(inner)]
    within = [[o * inner + i for i in range(inner)] for o in range(outer)]
    by_head = by_head.reshape(outer, per_device, tok_rows, head_width)
    if outer > 1:
        by_head = lax.all_to_all(by_head, "sp", 0, 0, axis_index_groups=across)
    kv = lax.all_gather(by_head[..., qdim:], "sp", axis=0, axis_index_groups=within)
    member = lax.rem(sp, inner).reshape(1)
    first_head = lax.div(sp, inner) * per_device
    attended = []
    for p in range(per_device):
        lam = lax.dynamic_slice_in_dim(lambdas, first_head + p, 1)
        attended.append(flash(by_head[:, p, :, :qdim], kv[:, :, p], member, lam, sub_gain))
    attended = jnp.stack(attended, axis=1)
    if outer > 1:
        attended = lax.all_to_all(attended, "sp", 0, 0, axis_index_groups=across)
    attended = attended.reshape(heads, tok_rows, vdim)

    pool_in = projected[:, heads * head_width :]
    halo = passed_along(pool_in[tok_rows - RIM_ROWS - 1 :], "sp", 1)
    extended = jnp.concatenate([halo, pool_in], axis=0).astype(jnp.float32)
    window_ids = (tp * groups + jnp.arange(groups, dtype=jnp.int32)) % len(WINDOWS)
    sums = trailing(extended, window_ids, group_dim)[RIM_ROWS + 1 :]
    spans = jnp.repeat(jnp.left_shift(2, window_ids), group_dim)
    positions = sp * tok_rows + jnp.arange(tok_rows, dtype=jnp.int32)
    count = jnp.minimum(positions[:, None] + 1, spans[None, :]).astype(jnp.float32)
    differ = (sums / count - pool_in.astype(jnp.float32)).astype(jnp.bfloat16)
    branch = []
    for g in range(groups):
        columns = slice(g * group_dim, (g + 1) * group_dim)
        pooled = jnp.dot(differ[:, columns], group_weight[g], preferred_element_type=jnp.float32)
        pooled = (pooled * pool_scale[columns][None, :]).astype(jnp.bfloat16)
        branch += [attended[g], pooled]
    branch = jnp.concatenate(branch, axis=1)
    partial = jnp.dot(branch, w_out_rows, preferred_element_type=jnp.float32)
    if n_tp == 2:
        half = tok_rows // 2
        keep = lax.dynamic_slice_in_dim(partial, tp * half, half, 0)
        send = lax.dynamic_slice_in_dim(partial, (1 - tp) * half, half, 0).astype(jnp.bfloat16)
        return (keep + lax.ppermute(send, "tp", swap).astype(jnp.float32)).astype(jnp.bfloat16)
    return lax.psum_scatter(partial.astype(jnp.bfloat16), "tp", scatter_dimension=0, tiled=True)


def solution(mesh):
    placed = (
        P("sp", "tp"),
        P("tp"),
        P("sp", "tp"),
        P("sp", "tp"),
        P("sp", "tp"),
        P("sp", "tp"),
        P("tp"),
        P(),
        P("tp", None, None),
        P("tp"),
        P("tp", "sp"),
    )
    return jax.shard_map(
        local, mesh=mesh, in_specs=placed, out_specs=P(("sp", "tp"), None), check_vma=False
    )
```

```python
import functools
import math

import jax
import jax.numpy as jnp
from jax import lax
from jax.experimental import pallas as pl
from jax.experimental.pallas import tpu as pltpu
from jax.sharding import PartitionSpec as P

EPSILON = 1e-06
NEG_LARGE = -1e30
WINDOWS = (2, 4, 8, 16)
RIM_ROWS = 15


def passed_along(block, axis, distance):
    devices = range(lax.axis_size(axis))
    route = [(i - distance, i) for i in devices if i - distance in devices]
    return lax.ppermute(block, axis, route)


def attend(inner, vdim, hdim, member_ref, lam_ref, q_ref, kv_ref, gain_ref, out_ref, acc_ref, max_ref):
    rows = q_ref.shape[1]
    block = pl.program_id(0)
    last = block * inner + member_ref[0]
    scale = 1.0 / math.sqrt(hdim)
    queries = (q_ref[0].astype(jnp.float32) * scale).astype(jnp.bfloat16)
    maps = (queries[:, :hdim], queries[:, hdim:])
    ones = jnp.ones((rows, vdim), jnp.bfloat16)
    acc_ref[...] = jnp.zeros_like(acc_ref)
    max_ref[...] = jnp.full_like(max_ref, NEG_LARGE)

    def step(g, masked):
        keys_values = kv_ref[lax.rem(g, inner), lax.div(g, inner)]
        values = jnp.concatenate([keys_values[:, 2 * hdim :], ones], axis=1)
        for m in range(2):
            keys = keys_values[:, m * hdim : (m + 1) * hdim]
            scores = lax.dot_general(
                maps[m], keys, (((1,), (1,)), ((), ())), preferred_element_type=jnp.float32
            )
            if masked:
                row = lax.broadcasted_iota(jnp.int32, scores.shape, 0)
                col = lax.broadcasted_iota(jnp.int32, scores.shape, 1)
                scores = jnp.where(col <= row, scores, NEG_LARGE)
            old_max = max_ref[m]
            new_max = jnp.maximum(old_max, jnp.max(scores, axis=1, keepdims=True))
            factor = jnp.exp(old_max - new_max)
            expo = jnp.exp(scores - new_max[:, :1])
            acc_ref[m] = acc_ref[m] * factor[:, :1] + jnp.dot(
                expo.astype(jnp.bfloat16), values, preferred_element_type=jnp.float32
            )
            max_ref[m] = new_max

    def body(g, carry):
        step(g, False)
        return carry

    lax.fori_loop(0, last, body, 0)
    step(last, True)
    first = acc_ref[0]
    second = acc_ref[1]
    mix = first[:, :vdim] / first[:, vdim:] - lam_ref[0] * (second[:, :vdim] / second[:, vdim:])
    mean_sq = jnp.mean(mix * mix, axis=1, keepdims=True)
    out_ref[0] = (mix * lax.rsqrt(mean_sq + EPSILON) * gain_ref[...]).astype(jnp.bfloat16)


def flash(q, kv, member, lam, sub_gain):
    inner, outer, rows, width = kv.shape
    qdim = q.shape[-1]
    vdim = width - qdim
    smem = pl.BlockSpec(memory_space=pltpu.SMEM)
    work = outer * rows * outer * rows * inner
    return pl.pallas_call(
        functools.partial(attend, inner, vdim, qdim // 2),
        grid=(outer,),
        out_shape=jax.ShapeDtypeStruct((outer, rows, vdim), jnp.bfloat16),
        in_specs=[
            smem,
            smem,
            pl.BlockSpec((1, rows, qdim), lambda b: (b, 0, 0)),
            pl.BlockSpec(memory_space=pltpu.VMEM),
            pl.BlockSpec(memory_space=pltpu.VMEM),
        ],
        out_specs=pl.BlockSpec((1, rows, vdim), lambda b: (b, 0, 0)),
        scratch_shapes=[
            pltpu.VMEM((2, rows, 2 * vdim), jnp.float32),
            pltpu.VMEM((2, rows, 128), jnp.float32),
        ],
        compiler_params=pltpu.CompilerParams(vmem_limit_bytes=56 * 2**20),
        cost_estimate=pl.CostEstimate(
            flops=4 * work * vdim, bytes_accessed=kv.size * 2, transcendentals=work
        ),
    )(member, lam, q, kv, sub_gain.reshape(1, -1))


def spread(n_sp, count, with_swap, *refs):
    weights, refs = refs[:count], refs[count:]
    mine, refs = refs[0], refs[1:]
    fulls, refs = refs[:count], refs[count:]
    theirs, refs = refs[0], refs[1:]
    up_send, up_recv, down_send, down_recv, y_send, y_recv, c_send, c_recv, own_sem, swap_sem = refs
    depth = n_sp // 4
    rows = weights[0].shape[0]
    sp = lax.axis_index("sp")
    z = lax.div(sp, 4)
    y = lax.rem(lax.div(sp, 2), 2)
    c = lax.rem(sp, 2)
    y_peer = z * 4 + (1 - y) * 2 + c
    c_peer = z * 4 + y * 2 + (1 - c)
    barrier = pltpu.get_barrier_semaphore()

    def greet(device):
        pl.semaphore_signal(barrier, 1, device_id=device, device_id_type=pl.DeviceIdType.MESH)

    greet({"sp": y_peer})
    greet({"sp": c_peer})
    greeted = 2
    if with_swap:
        greet({"tp": 1 - lax.axis_index("tp")})
        greeted = 3

    @pl.when(z > 0)
    def _():
        greet({"sp": sp - 4})

    @pl.when(z < depth - 1)
    def _():
        greet({"sp": sp + 4})

    in_line = jnp.where(z > 0, 1, 0) + jnp.where(z < depth - 1, 1, 0)
    pl.semaphore_wait(barrier, greeted + in_line)

    def slot(a, zz, yy, cc):
        start = pl.multiple_of((zz * 4 + yy * 2 + cc) * rows, rows)
        return fulls[a].at[pl.ds(start, rows), :]

    def remote(src, dst, send, recv, device):
        return pltpu.make_async_remote_copy(
            src_ref=src,
            dst_ref=dst,
            send_sem=send,
            recv_sem=recv,
            device_id=device,
            device_id_type=pl.DeviceIdType.MESH,
        )

    def line_copy(side, k, a, src):
        sends, recvs = (up_send, up_recv) if side > 0 else (down_send, down_recv)
        there = slot(a, z - side * k, y, c)
        return remote(
            there if src is None else src,
            there,
            sends.at[k, a],
            recvs.at[k + 1, a],
            {"sp": sp + 4 * side},
        )

    def y_copy(zz, yy, a, src):
        there = slot(a, zz, yy, c)
        src = there if src is None else src
        return remote(src, there, y_send.at[zz, a], y_recv.at[zz, a], {"sp": y_peer})

    def c_copy(zz, yy, cc, a, src):
        there = slot(a, zz, yy, cc)
        src = there if src is None else src
        return remote(src, there, c_send.at[zz, yy, a], c_recv.at[zz, yy, a], {"sp": c_peer})

    def can_go(side):
        return z < depth - 1 if side > 0 else z > 0

    def came(side, k):
        return z >= k if side > 0 else z + k <= depth - 1

    if with_swap:
        swap = remote(
            mine, theirs, swap_sem.at[0], swap_sem.at[1], {"tp": 1 - lax.axis_index("tp")}
        )
        swap.start()
    for a in range(count):
        for side in (1, -1):

            @pl.when(can_go(side))
            def _():
                line_copy(side, 0, a, weights[a]).start()

        y_copy(z, y, a, weights[a]).start()
    for a in range(count):
        c_copy(z, y, c, a, weights[a]).start()
        pltpu.make_async_copy(weights[a], slot(a, z, y, c), own_sem.at[a]).start()

    def from_pair(zz):
        for a in range(count):
            y_copy(zz, 1 - y, a, None).wait_recv()
            c_copy(zz, 1 - y, c, a, None).start()

    def relay(k, carry):
        for side in (1, -1):
            recvs = up_recv if side > 0 else down_recv

            @pl.when(came(side, k))
            def _():
                zz = z - side * k
                for a in range(count):
                    there = slot(a, zz, y, c)
                    remote(there, there, up_send.at[0, a], recvs.at[k, a], {"sp": y_peer}).wait_recv()

                    @pl.when(can_go(side))
                    def _():
                        line_copy(side, k, a, None).start()

                    y_copy(zz, y, a, None).start()
                    c_copy(zz, y, c, a, None).start()

        @pl.when(k == 1)
        def _():
            from_pair(z)

        for side in (1, -1):

            @pl.when((k > 1) & came(side, k - 1))
            def _():
                from_pair(z - side * (k - 1))

        return carry

    lax.fori_loop(1, depth, relay, 0)
    if depth == 1:
        from_pair(z)
    for side in (1, -1):
        if depth > 1:

            @pl.when(came(side, depth - 1))
            def _():
                from_pair(z - side * (depth - 1))

    def drain(zz, carry):
        for a in range(count):
            y_copy(zz, y, a, None).wait_send()
            for yy in range(2):
                c_copy(zz, yy, 1 - c, a, None).wait_recv()
                c_copy(zz, yy, c, a, None).wait_send()
        return carry

    lax.fori_loop(0, depth, drain, 0)

    def drain_line(k, carry):
        for side in (1, -1):

            @pl.when(came(side, k) & can_go(side))
            def _():
                for a in range(count):
                    line_copy(side, k, a, None).wait_send()

        return carry

    lax.fori_loop(0, depth, drain_line, 0)
    for a in range(count):
        pltpu.make_async_copy(weights[a], slot(a, z, y, c), own_sem.at[a]).wait()
    if with_swap:
        swap.wait()


def gather_weights(weights, mine, with_swap):
    n_sp = lax.axis_size("sp")
    count = len(weights)
    depth = n_sp // 4
    sems = pltpu.SemaphoreType.DMA
    any_spec = pl.BlockSpec(memory_space=pl.ANY)
    vmem_spec = pl.BlockSpec(memory_space=pltpu.VMEM)
    shapes = [jax.ShapeDtypeStruct((n_sp * w.shape[0], w.shape[1]), w.dtype) for w in weights]
    shapes.append(jax.ShapeDtypeStruct(mine.shape, mine.dtype))
    moved = sum(w.size for w in weights) * 2 * n_sp
    return pl.pallas_call(
        functools.partial(spread, n_sp, count, with_swap),
        out_shape=shapes,
        in_specs=[vmem_spec] * (count + 1),
        out_specs=[any_spec] * (count + 1),
        scratch_shapes=[
            sems((depth + 1, count)),
            sems((depth + 1, count)),
            sems((depth + 1, count)),
            sems((depth + 1, count)),
            sems((depth, count)),
            sems((depth, count)),
            sems((depth, 2, count)),
            sems((depth, 2, count)),
            sems((count,)),
            sems((2,)),
        ],
        compiler_params=pltpu.CompilerParams(collective_id=0, has_side_effects=True),
        cost_estimate=pl.CostEstimate(flops=10**10, bytes_accessed=moved, transcendentals=0),
    )(*weights, mine)


def trailing(x, window_ids, group_dim):
    column_window = jnp.repeat(window_ids, group_dim)[None, :]
    running = x
    picked = jnp.zeros_like(x)
    for slot, span in enumerate(WINDOWS):
        half = span // 2
        running = running + jnp.pad(running[:-half], ((half, 0), (0, 0)))
        picked = jnp.where(column_window == slot, running, picked)
    return picked


def local(
    tokens,
    pre_gain,
    w_query,
    w_key,
    w_value,
    w_pool,
    lambdas,
    sub_gain,
    group_weight,
    pool_scale,
    w_out,
):
    n_tp = lax.axis_size("tp")
    n_sp = lax.axis_size("sp")
    tp = lax.axis_index("tp")
    sp = lax.axis_index("sp")
    tok_rows = tokens.shape[0]
    model_width = tokens.shape[1] * n_tp
    heads = lambdas.shape[0]
    qdim = w_query.shape[1] // heads
    vdim = w_value.shape[1] // heads
    groups = group_weight.shape[0]
    group_dim = group_weight.shape[1]
    head_width = 2 * qdim + vdim
    outer = math.gcd(n_sp, heads)
    inner = n_sp // outer
    per_device = heads // outer

    features = tokens.astype(jnp.float32)
    mine = (features * pre_gain.astype(jnp.float32)[None, :]).astype(jnp.bfloat16)
    squares = jnp.sum(features * features, axis=1, keepdims=True)
    swap = [(0, 1), (1, 0)]
    weights = [w_query, w_key, w_value, w_pool]
    if n_sp % 4 == 0:
        *weights, theirs = gather_weights(weights, mine, n_tp == 2)
    else:
        weights = [lax.all_gather(w, "sp", axis=0, tiled=True) for w in weights]
        theirs = lax.ppermute(mine, "tp", swap) if n_tp == 2 else mine
    w_sorted = w_out.reshape(heads, 2, vdim, -1).swapaxes(0, 1).reshape(w_out.shape)
    w_sorted, weights = lax.optimization_barrier((w_sorted, weights))
    w_out_rows = lax.all_gather(w_sorted, "sp", axis=1, tiled=True)
    if n_tp == 2:
        squares = squares + lax.ppermute(squares, "tp", swap)
        scaled = jnp.concatenate(
            [jnp.where(tp == 0, mine, theirs), jnp.where(tp == 0, theirs, mine)], axis=1
        )
    else:
        scaled = lax.all_gather(mine, "tp", axis=1, tiled=True)
        squares = lax.psum(squares, "tp")
    inverse = lax.rsqrt(squares / model_width + EPSILON)
    queries, key_rows, values, pool_in = [
        (jnp.dot(scaled, w, preferred_element_type=jnp.float32) * inverse).astype(jnp.bfloat16)
        for w in weights
    ]
    by_head = jnp.concatenate(
        [
            x.reshape(tok_rows, heads, -1).swapaxes(0, 1)
            for x in (queries, key_rows, values)
        ],
        axis=2,
    )
    across = [[o * inner + i for o in range(outer)] for i in range(inner)]
    within = [[o * inner + i for i in range(inner)] for o in range(outer)]
    by_head = by_head.reshape(outer, per_device, tok_rows, head_width)
    if outer > 1:
        by_head = lax.all_to_all(by_head, "sp", 0, 0, axis_index_groups=across)
    kv = lax.all_gather(by_head[..., qdim:], "sp", axis=0, axis_index_groups=within)
    member = lax.rem(sp, inner).reshape(1)
    first_head = lax.div(sp, inner) * per_device
    attended = []
    for p in range(per_device):
        lam = lax.dynamic_slice_in_dim(lambdas, first_head + p, 1)
        attended.append(flash(by_head[:, p, :, :qdim], kv[:, :, p], member, lam, sub_gain))
    attended = jnp.stack(attended, axis=1)
    if outer > 1:
        attended = lax.all_to_all(attended, "sp", 0, 0, axis_index_groups=across)
    attended = attended.reshape(heads, tok_rows, vdim)

    halo = passed_along(pool_in[tok_rows - RIM_ROWS - 1 :], "sp", 1)
    extended = jnp.concatenate([halo, pool_in], axis=0).astype(jnp.float32)
    window_ids = (tp * groups + jnp.arange(groups, dtype=jnp.int32)) % len(WINDOWS)
    sums = trailing(extended, window_ids, group_dim)[RIM_ROWS + 1 :]
    spans = jnp.repeat(jnp.left_shift(2, window_ids), group_dim)
    positions = sp * tok_rows + jnp.arange(tok_rows, dtype=jnp.int32)
    count = jnp.minimum(positions[:, None] + 1, spans[None, :]).astype(jnp.float32)
    differ = (sums / count - pool_in.astype(jnp.float32)).astype(jnp.bfloat16)
    pooled = jnp.einsum(
        "tgc,gcd->tgd",
        differ.reshape(tok_rows, groups, group_dim),
        group_weight,
        preferred_element_type=jnp.float32,
    )
    pooled = (pooled * pool_scale.reshape(groups, group_dim)).astype(jnp.bfloat16)
    branch = jnp.concatenate(
        [attended.swapaxes(0, 1).reshape(tok_rows, -1), pooled.reshape(tok_rows, -1)], axis=1
    )
    partial = jnp.dot(branch, w_out_rows, preferred_element_type=jnp.float32)
    if n_tp == 2:
        half = tok_rows // 2
        keep = lax.dynamic_slice_in_dim(partial, tp * half, half, 0)
        send = lax.dynamic_slice_in_dim(partial, (1 - tp) * half, half, 0).astype(jnp.bfloat16)
        return (keep + lax.ppermute(send, "tp", swap).astype(jnp.float32)).astype(jnp.bfloat16)
    return lax.psum_scatter(partial.astype(jnp.bfloat16), "tp", scatter_dimension=0, tiled=True)


def solution(mesh):
    placed = (
        P("sp", "tp"),
        P("tp"),
        P("sp", "tp"),
        P("sp", "tp"),
        P("sp", "tp"),
        P("sp", "tp"),
        P("tp"),
        P(),
        P("tp", None, None),
        P("tp"),
        P("tp", "sp"),
    )
    return jax.shard_map(
        local, mesh=mesh, in_specs=placed, out_specs=P(("sp", "tp"), None), check_vma=False
    )
```

```python
import functools
import math

import jax
import jax.numpy as jnp
from jax import lax
from jax.experimental import pallas as pl
from jax.experimental.pallas import tpu as pltpu
from jax.sharding import PartitionSpec as P

EPSILON = 1e-06
NEG_LARGE = -1e30
WINDOWS = (2, 4, 8, 16)
RIM_ROWS = 15


def passed_along(block, axis, distance):
    devices = range(lax.axis_size(axis))
    route = [(i - distance, i) for i in devices if i - distance in devices]
    return lax.ppermute(block, axis, route)


def attend(inner, vdim, hdim, member_ref, lam_ref, q_ref, kv_ref, gain_ref, out_ref, acc_ref, max_ref):
    rows = q_ref.shape[1]
    block = pl.program_id(0)
    last = block * inner + member_ref[0]
    scale = 1.0 / math.sqrt(hdim)
    queries = (q_ref[0].astype(jnp.float32) * scale).astype(jnp.bfloat16)
    maps = (queries[:, :hdim], queries[:, hdim:])
    ones = jnp.ones((rows, vdim), jnp.bfloat16)
    acc_ref[...] = jnp.zeros_like(acc_ref)
    max_ref[...] = jnp.full_like(max_ref, NEG_LARGE)

    def step(g, masked):
        keys_values = kv_ref[lax.rem(g, inner), lax.div(g, inner)]
        values = jnp.concatenate([keys_values[:, 2 * hdim :], ones], axis=1)
        for m in range(2):
            keys = keys_values[:, m * hdim : (m + 1) * hdim]
            scores = lax.dot_general(
                maps[m], keys, (((1,), (1,)), ((), ())), preferred_element_type=jnp.float32
            )
            if masked:
                row = lax.broadcasted_iota(jnp.int32, scores.shape, 0)
                col = lax.broadcasted_iota(jnp.int32, scores.shape, 1)
                scores = jnp.where(col <= row, scores, NEG_LARGE)
            old_max = max_ref[m]
            new_max = jnp.maximum(old_max, jnp.max(scores, axis=1, keepdims=True))
            factor = jnp.exp(old_max - new_max)
            expo = jnp.exp(scores - new_max[:, :1])
            acc_ref[m] = acc_ref[m] * factor[:, :1] + jnp.dot(
                expo.astype(jnp.bfloat16), values, preferred_element_type=jnp.float32
            )
            max_ref[m] = new_max

    def body(g, carry):
        step(g, False)
        return carry

    lax.fori_loop(0, last, body, 0)
    step(last, True)
    first = acc_ref[0]
    second = acc_ref[1]
    mix = first[:, :vdim] / first[:, vdim:] - lam_ref[0] * (second[:, :vdim] / second[:, vdim:])
    mean_sq = jnp.mean(mix * mix, axis=1, keepdims=True)
    out_ref[0] = (mix * lax.rsqrt(mean_sq + EPSILON) * gain_ref[...]).astype(jnp.bfloat16)


def flash(q, kv, member, lam, sub_gain):
    inner, outer, rows, width = kv.shape
    qdim = q.shape[-1]
    vdim = width - qdim
    smem = pl.BlockSpec(memory_space=pltpu.SMEM)
    work = outer * rows * outer * rows * inner
    return pl.pallas_call(
        functools.partial(attend, inner, vdim, qdim // 2),
        grid=(outer,),
        out_shape=jax.ShapeDtypeStruct((outer, rows, vdim), jnp.bfloat16),
        in_specs=[
            smem,
            smem,
            pl.BlockSpec((1, rows, qdim), lambda b: (b, 0, 0)),
            pl.BlockSpec(memory_space=pltpu.VMEM),
            pl.BlockSpec(memory_space=pltpu.VMEM),
        ],
        out_specs=pl.BlockSpec((1, rows, vdim), lambda b: (b, 0, 0)),
        scratch_shapes=[
            pltpu.VMEM((2, rows, 2 * vdim), jnp.float32),
            pltpu.VMEM((2, rows, 128), jnp.float32),
        ],
        compiler_params=pltpu.CompilerParams(vmem_limit_bytes=56 * 2**20),
        cost_estimate=pl.CostEstimate(
            flops=4 * work * vdim, bytes_accessed=kv.size * 2, transcendentals=work
        ),
    )(member, lam, q, kv, sub_gain.reshape(1, -1))


def attend_members(hdim, lam_ref, q_ref, own_ref, gain_ref, out_ref, held, acc_ref, max_ref, send, recv):
    outer, rows, _ = q_ref.shape
    vdim = own_ref.shape[2] - 2 * hdim
    sp = lax.axis_index("sp")
    member = lax.rem(sp, 4)
    y = lax.div(member, 2)
    c = lax.rem(member, 2)
    y_peer = sp + 2 - 4 * y
    c_peer = sp + 1 - 2 * c
    barrier = pltpu.get_barrier_semaphore()
    for peer in (y_peer, c_peer):
        pl.semaphore_signal(
            barrier, 1, device_id={"sp": peer}, device_id_type=pl.DeviceIdType.MESH
        )
    pl.semaphore_wait(barrier, 2)

    def remote(src, index, peer):
        return pltpu.make_async_remote_copy(
            src_ref=src,
            dst_ref=held.at[index],
            send_sem=send.at[index],
            recv_sem=recv.at[index],
            device_id={"sp": peer},
            device_id_type=pl.DeviceIdType.MESH,
        )

    across = remote(own_ref, 1, y_peer)
    beside = remote(own_ref, 0, c_peer)
    onward = remote(held.at[1], 2, c_peer)
    across.start()
    beside.start()
    acc_ref[...] = jnp.zeros_like(acc_ref)
    max_ref[...] = jnp.full_like(max_ref, NEG_LARGE)
    scale = 1.0 / math.sqrt(hdim)

    def visit(ref, other):
        shift = (member - other) * rows
        for block in range(outer):
            queries = (q_ref[block].astype(jnp.float32) * scale).astype(jnp.bfloat16)
            length = (block + 1) * rows
            keys_values = ref[: block + 1].reshape(length, 2 * hdim + vdim)
            values = jnp.concatenate(
                [keys_values[:, 2 * hdim :], jnp.ones((length, vdim), jnp.bfloat16)], axis=1
            )
            for m in range(2):
                scores = lax.dot_general(
                    queries[:, m * hdim : (m + 1) * hdim],
                    keys_values[:, m * hdim : (m + 1) * hdim],
                    (((1,), (1,)), ((), ())),
                    preferred_element_type=jnp.float32,
                )
                edge = scores[:, block * rows :]
                row = lax.broadcasted_iota(jnp.int32, edge.shape, 0)
                col = lax.broadcasted_iota(jnp.int32, edge.shape, 1)
                edge = jnp.where(col <= row + shift, edge, NEG_LARGE)
                if block > 0:
                    scores = jnp.concatenate([scores[:, : block * rows], edge], axis=1)
                else:
                    scores = edge
                old_max = max_ref[block, m]
                new_max = jnp.maximum(old_max, jnp.max(scores, axis=1, keepdims=True))
                factor = jnp.exp(old_max - new_max)
                expo = jnp.exp(scores - new_max[:, :1])
                acc_ref[block, m] = acc_ref[block, m] * factor[:, :1] + jnp.dot(
                    expo.astype(jnp.bfloat16), values, preferred_element_type=jnp.float32
                )
                max_ref[block, m] = new_max

    visit(own_ref, member)

    def arrived(j, carry):
        @pl.when(j == 0)
        def _():
            beside.wait_recv()

        @pl.when(j == 1)
        def _():
            across.wait_recv()
            onward.start()

        @pl.when(j == 2)
        def _():
            onward.wait_recv()

        other_y = jnp.where(j >= 1, 1 - y, y)
        other_c = jnp.where(j == 1, c, 1 - c)
        visit(held.at[j], 2 * other_y + other_c)
        return carry

    lax.fori_loop(0, 3, arrived, 0)
    for copy in (across, beside, onward):
        copy.wait_send()
    for block in range(outer):
        first = acc_ref[block, 0]
        second = acc_ref[block, 1]
        mix = first[:, :vdim] / first[:, vdim:]
        mix = mix - lam_ref[0] * (second[:, :vdim] / second[:, vdim:])
        mean_sq = jnp.mean(mix * mix, axis=1, keepdims=True)
        normed = mix * lax.rsqrt(mean_sq + EPSILON) * gain_ref[...]
        out_ref[block] = normed.astype(jnp.bfloat16)


def flash_members(q, kv, lam, sub_gain):
    outer, rows, width = kv.shape
    qdim = q.shape[-1]
    vdim = width - qdim
    vmem = pl.BlockSpec(memory_space=pltpu.VMEM)
    work = 4 * outer * rows * outer * rows
    return pl.pallas_call(
        functools.partial(attend_members, qdim // 2),
        out_shape=jax.ShapeDtypeStruct((outer, rows, vdim), jnp.bfloat16),
        in_specs=[pl.BlockSpec(memory_space=pltpu.SMEM), vmem, vmem, vmem],
        out_specs=vmem,
        scratch_shapes=[
            pltpu.VMEM((3, outer, rows, width), jnp.bfloat16),
            pltpu.VMEM((outer, 2, rows, 2 * vdim), jnp.float32),
            pltpu.VMEM((outer, 2, rows, 128), jnp.float32),
            pltpu.SemaphoreType.DMA((3,)),
            pltpu.SemaphoreType.DMA((3,)),
        ],
        compiler_params=pltpu.CompilerParams(
            vmem_limit_bytes=56 * 2**20, collective_id=1, has_side_effects=True
        ),
        cost_estimate=pl.CostEstimate(
            flops=4 * work * vdim, bytes_accessed=4 * kv.size * 2, transcendentals=work
        ),
    )(lam, q, kv, sub_gain.reshape(1, -1))


def spread(n_sp, count, with_swap, *refs):
    weights, refs = refs[:count], refs[count:]
    mine, refs = refs[0], refs[1:]
    fulls, refs = refs[:count], refs[count:]
    theirs, refs = refs[0], refs[1:]
    up_send, up_recv, down_send, down_recv, y_send, y_recv, c_send, c_recv, own_sem, swap_sem = refs
    depth = n_sp // 4
    rows = weights[0].shape[0]
    sp = lax.axis_index("sp")
    z = lax.div(sp, 4)
    y = lax.rem(lax.div(sp, 2), 2)
    c = lax.rem(sp, 2)
    y_peer = z * 4 + (1 - y) * 2 + c
    c_peer = z * 4 + y * 2 + (1 - c)
    barrier = pltpu.get_barrier_semaphore()

    def greet(device):
        pl.semaphore_signal(barrier, 1, device_id=device, device_id_type=pl.DeviceIdType.MESH)

    greet({"sp": y_peer})
    greet({"sp": c_peer})
    greeted = 2
    if with_swap:
        greet({"tp": 1 - lax.axis_index("tp")})
        greeted = 3

    @pl.when(z > 0)
    def _():
        greet({"sp": sp - 4})

    @pl.when(z < depth - 1)
    def _():
        greet({"sp": sp + 4})

    in_line = jnp.where(z > 0, 1, 0) + jnp.where(z < depth - 1, 1, 0)
    pl.semaphore_wait(barrier, greeted + in_line)

    def slot(a, zz, yy, cc):
        start = pl.multiple_of((zz * 4 + yy * 2 + cc) * rows, rows)
        return fulls[a].at[pl.ds(start, rows), :]

    def remote(src, dst, send, recv, device):
        return pltpu.make_async_remote_copy(
            src_ref=src,
            dst_ref=dst,
            send_sem=send,
            recv_sem=recv,
            device_id=device,
            device_id_type=pl.DeviceIdType.MESH,
        )

    def line_copy(side, k, a, src):
        sends, recvs = (up_send, up_recv) if side > 0 else (down_send, down_recv)
        there = slot(a, z - side * k, y, c)
        return remote(
            there if src is None else src,
            there,
            sends.at[k, a],
            recvs.at[k + 1, a],
            {"sp": sp + 4 * side},
        )

    def y_copy(zz, yy, a, src):
        there = slot(a, zz, yy, c)
        src = there if src is None else src
        return remote(src, there, y_send.at[zz, a], y_recv.at[zz, a], {"sp": y_peer})

    def c_copy(zz, yy, cc, a, src):
        there = slot(a, zz, yy, cc)
        src = there if src is None else src
        return remote(src, there, c_send.at[zz, yy, a], c_recv.at[zz, yy, a], {"sp": c_peer})

    def can_go(side):
        return z < depth - 1 if side > 0 else z > 0

    def came(side, k):
        return z >= k if side > 0 else z + k <= depth - 1

    if with_swap:
        swap = remote(
            mine, theirs, swap_sem.at[0], swap_sem.at[1], {"tp": 1 - lax.axis_index("tp")}
        )
        swap.start()
    for a in range(count):
        for side in (1, -1):

            @pl.when(can_go(side))
            def _():
                line_copy(side, 0, a, weights[a]).start()

        y_copy(z, y, a, weights[a]).start()
    for a in range(count):
        c_copy(z, y, c, a, weights[a]).start()
        pltpu.make_async_copy(weights[a], slot(a, z, y, c), own_sem.at[a]).start()

    def from_pair(zz):
        for a in range(count):
            y_copy(zz, 1 - y, a, None).wait_recv()
            c_copy(zz, 1 - y, c, a, None).start()

    def relay(k, carry):
        for side in (1, -1):
            recvs = up_recv if side > 0 else down_recv

            @pl.when(came(side, k))
            def _():
                zz = z - side * k
                for a in range(count):
                    there = slot(a, zz, y, c)
                    remote(there, there, up_send.at[0, a], recvs.at[k, a], {"sp": y_peer}).wait_recv()

                    @pl.when(can_go(side))
                    def _():
                        line_copy(side, k, a, None).start()

                    y_copy(zz, y, a, None).start()
                    c_copy(zz, y, c, a, None).start()

        @pl.when(k == 1)
        def _():
            from_pair(z)

        for side in (1, -1):

            @pl.when((k > 1) & came(side, k - 1))
            def _():
                from_pair(z - side * (k - 1))

        return carry

    lax.fori_loop(1, depth, relay, 0)
    if depth == 1:
        from_pair(z)
    for side in (1, -1):
        if depth > 1:

            @pl.when(came(side, depth - 1))
            def _():
                from_pair(z - side * (depth - 1))

    def drain(zz, carry):
        for a in range(count):
            y_copy(zz, y, a, None).wait_send()
            for yy in range(2):
                c_copy(zz, yy, 1 - c, a, None).wait_recv()
                c_copy(zz, yy, c, a, None).wait_send()
        return carry

    lax.fori_loop(0, depth, drain, 0)

    def drain_line(k, carry):
        for side in (1, -1):

            @pl.when(came(side, k) & can_go(side))
            def _():
                for a in range(count):
                    line_copy(side, k, a, None).wait_send()

        return carry

    lax.fori_loop(0, depth, drain_line, 0)
    for a in range(count):
        pltpu.make_async_copy(weights[a], slot(a, z, y, c), own_sem.at[a]).wait()
    if with_swap:
        swap.wait()


def gather_weights(weights, mine, with_swap):
    n_sp = lax.axis_size("sp")
    count = len(weights)
    depth = n_sp // 4
    sems = pltpu.SemaphoreType.DMA
    any_spec = pl.BlockSpec(memory_space=pl.ANY)
    vmem_spec = pl.BlockSpec(memory_space=pltpu.VMEM)
    shapes = [jax.ShapeDtypeStruct((n_sp * w.shape[0], w.shape[1]), w.dtype) for w in weights]
    shapes.append(jax.ShapeDtypeStruct(mine.shape, mine.dtype))
    moved = sum(w.size for w in weights) * 2 * n_sp
    return pl.pallas_call(
        functools.partial(spread, n_sp, count, with_swap),
        out_shape=shapes,
        in_specs=[vmem_spec] * (count + 1),
        out_specs=[any_spec] * (count + 1),
        scratch_shapes=[
            sems((depth + 1, count)),
            sems((depth + 1, count)),
            sems((depth + 1, count)),
            sems((depth + 1, count)),
            sems((depth, count)),
            sems((depth, count)),
            sems((depth, 2, count)),
            sems((depth, 2, count)),
            sems((count,)),
            sems((2,)),
        ],
        compiler_params=pltpu.CompilerParams(collective_id=0, has_side_effects=True),
        cost_estimate=pl.CostEstimate(flops=10**10, bytes_accessed=moved, transcendentals=0),
    )(*weights, mine)


def trailing(x, window_ids, group_dim):
    column_window = jnp.repeat(window_ids, group_dim)[None, :]
    running = x
    picked = jnp.zeros_like(x)
    for slot, span in enumerate(WINDOWS):
        half = span // 2
        running = running + jnp.pad(running[:-half], ((half, 0), (0, 0)))
        picked = jnp.where(column_window == slot, running, picked)
    return picked


def local(
    tokens,
    pre_gain,
    w_query,
    w_key,
    w_value,
    w_pool,
    lambdas,
    sub_gain,
    group_weight,
    pool_scale,
    w_out,
):
    n_tp = lax.axis_size("tp")
    n_sp = lax.axis_size("sp")
    tp = lax.axis_index("tp")
    sp = lax.axis_index("sp")
    tok_rows = tokens.shape[0]
    model_width = tokens.shape[1] * n_tp
    heads = lambdas.shape[0]
    qdim = w_query.shape[1] // heads
    vdim = w_value.shape[1] // heads
    groups = group_weight.shape[0]
    group_dim = group_weight.shape[1]
    head_width = 2 * qdim + vdim
    outer = math.gcd(n_sp, heads)
    inner = n_sp // outer
    per_device = heads // outer

    features = tokens.astype(jnp.float32)
    mine = (features * pre_gain.astype(jnp.float32)[None, :]).astype(jnp.bfloat16)
    squares = jnp.sum(features * features, axis=1, keepdims=True)
    swap = [(0, 1), (1, 0)]
    weights = [w_query, w_key, w_value, w_pool]
    if n_sp % 4 == 0:
        *weights, theirs = gather_weights(weights, mine, n_tp == 2)
    else:
        weights = [lax.all_gather(w, "sp", axis=0, tiled=True) for w in weights]
        theirs = lax.ppermute(mine, "tp", swap) if n_tp == 2 else mine
    w_sorted = w_out.reshape(heads, 2, vdim, -1).swapaxes(0, 1).reshape(w_out.shape)
    w_sorted, weights = lax.optimization_barrier((w_sorted, weights))
    w_out_rows = lax.all_gather(w_sorted, "sp", axis=1, tiled=True)
    if n_tp == 2:
        squares = squares + lax.ppermute(squares, "tp", swap)
        scaled = jnp.concatenate(
            [jnp.where(tp == 0, mine, theirs), jnp.where(tp == 0, theirs, mine)], axis=1
        )
    else:
        scaled = lax.all_gather(mine, "tp", axis=1, tiled=True)
        squares = lax.psum(squares, "tp")
    inverse = lax.rsqrt(squares / model_width + EPSILON)
    queries, key_rows, values, pool_in = [
        (jnp.dot(scaled, w, preferred_element_type=jnp.float32) * inverse).astype(jnp.bfloat16)
        for w in weights
    ]
    by_head = jnp.concatenate(
        [
            x.reshape(tok_rows, heads, -1).swapaxes(0, 1)
            for x in (queries, key_rows, values)
        ],
        axis=2,
    )
    across = [[o * inner + i for o in range(outer)] for i in range(inner)]
    within = [[o * inner + i for i in range(inner)] for o in range(outer)]
    by_head = by_head.reshape(outer, per_device, tok_rows, head_width)
    if outer > 1:
        by_head = lax.all_to_all(by_head, "sp", 0, 0, axis_index_groups=across)
    first_head = lax.div(sp, inner) * per_device
    attended = []
    if inner == 4 and per_device == 1:
        lam = lax.dynamic_slice_in_dim(lambdas, first_head, 1)
        attended.append(
            flash_members(by_head[:, 0, :, :qdim], by_head[:, 0, :, qdim:], lam, sub_gain)
        )
    else:
        kv = lax.all_gather(by_head[..., qdim:], "sp", axis=0, axis_index_groups=within)
        member = lax.rem(sp, inner).reshape(1)
        for p in range(per_device):
            lam = lax.dynamic_slice_in_dim(lambdas, first_head + p, 1)
            attended.append(flash(by_head[:, p, :, :qdim], kv[:, :, p], member, lam, sub_gain))
    attended = jnp.stack(attended, axis=1)
    if outer > 1:
        attended = lax.all_to_all(attended, "sp", 0, 0, axis_index_groups=across)
    attended = attended.reshape(heads, tok_rows, vdim)

    halo = passed_along(pool_in[tok_rows - RIM_ROWS - 1 :], "sp", 1)
    extended = jnp.concatenate([halo, pool_in], axis=0).astype(jnp.float32)
    window_ids = (tp * groups + jnp.arange(groups, dtype=jnp.int32)) % len(WINDOWS)
    sums = trailing(extended, window_ids, group_dim)[RIM_ROWS + 1 :]
    spans = jnp.repeat(jnp.left_shift(2, window_ids), group_dim)
    positions = sp * tok_rows + jnp.arange(tok_rows, dtype=jnp.int32)
    count = jnp.minimum(positions[:, None] + 1, spans[None, :]).astype(jnp.float32)
    differ = (sums / count - pool_in.astype(jnp.float32)).astype(jnp.bfloat16)
    pooled = jnp.einsum(
        "tgc,gcd->tgd",
        differ.reshape(tok_rows, groups, group_dim),
        group_weight,
        preferred_element_type=jnp.float32,
    )
    pooled = (pooled * pool_scale.reshape(groups, group_dim)).astype(jnp.bfloat16)
    branch = jnp.concatenate(
        [attended.swapaxes(0, 1).reshape(tok_rows, -1), pooled.reshape(tok_rows, -1)], axis=1
    )
    if n_tp == 2:
        half = tok_rows // 2
        send = lax.dynamic_slice_in_dim(branch, (1 - tp) * half, half, 0)
        send = jnp.dot(send, w_out_rows, preferred_element_type=jnp.float32).astype(jnp.bfloat16)
        got = lax.ppermute(send, "tp", swap)
        keep = lax.dynamic_slice_in_dim(branch, tp * half, half, 0)
        keep = jnp.dot(keep, w_out_rows, preferred_element_type=jnp.float32)
        return (keep + got.astype(jnp.float32)).astype(jnp.bfloat16)
    partial = jnp.dot(branch, w_out_rows, preferred_element_type=jnp.float32)
    return lax.psum_scatter(partial.astype(jnp.bfloat16), "tp", scatter_dimension=0, tiled=True)


def solution(mesh):
    placed = (
        P("sp", "tp"),
        P("tp"),
        P("sp", "tp"),
        P("sp", "tp"),
        P("sp", "tp"),
        P("sp", "tp"),
        P("tp"),
        P(),
        P("tp", None, None),
        P("tp"),
        P("tp", "sp"),
    )
    return jax.shard_map(
        local, mesh=mesh, in_specs=placed, out_specs=P(("sp", "tp"), None), check_vma=False
    )
```
